32 devices in a mesh: kv: 16 (over z, y, x), tp: 2 (over core).
Axes of the slice: x: 2, y: 2, z: 4, core: 2. Of those that a mesh axis runs over, the one named last changes fastest.
Arguments:
- tokens: bfloat16 [32, 4096], P(None, 'kv'), may hold values from -16 to 16
- mix_gain: bfloat16 [4096], P('kv'), may hold values from 0.099609375 to 1.8984375
- ffn_gain: bfloat16 [4096], P('kv'), may hold values from 0.099609375 to 1.8984375
- w_query: bfloat16 [4096, 2048], P('kv', 'tp'), may hold values from -0.09375 to 0.09375
- w_key: bfloat16 [4096, 2048], P('kv', 'tp'), may hold values from -0.09375 to 0.09375
- w_value: bfloat16 [4096, 4096], P('kv', 'tp'), may hold values from -0.09375 to 0.09375
- w_gate: bfloat16 [4096, 4096], P('kv', 'tp'), may hold values from -0.09375 to 0.09375
- w_decay: bfloat16 [4096, 2048], P('kv', 'tp'), may hold values from -0.375 to 0.375
- decay_bias: float32 [2048], P('tp'), may hold values from -7 to 4
- head_gain: bfloat16 [512], replicated, may hold values from 0.099609375 to 1.8984375
- w_output: bfloat16 [4096, 4096], P('tp', 'kv'), may hold values from -0.09375 to 0.09375
- w_ffgate: bfloat16 [4096, 11008], P('kv', 'tp'), may hold values from -0.09375 to 0.09375
- w_ffup: bfloat16 [4096, 11008], P('kv', 'tp'), may hold values from -0.09375 to 0.09375
- w_down: bfloat16 [11008, 4096], P('tp', 'kv'), may hold values from -0.0546875 to 0.0546875
- state: float32 [32, 8, 256, 512], P('kv', 'tp'), may hold values from -6 to 6
Outputs:
- mixed: bfloat16 [32, 4096], P(None, 'kv')
- new_state: float32 [32, 8, 256, 512], P('kv', 'tp')
The draws below stay inside these ranges and needn't reach their ends.
All inputs are finite; a program needn't handle non-finite values.
Results may differ from the reference program's by a relative error of at most 0.015.
Values may be sent and summed in bfloat16 or wider, within the bound.
A program may use at most 64 MiB of HBM per device.

```python
import jax
import jax.numpy as jnp
from jax import lax

D = 4096
HEADS = 8
DK = 256
DV = 512
FF = 11008
SEQS = 32
GROUPS = 2


def draw_tokens(key, part):
    column = jnp.arange(D, dtype=jnp.float32) / D
    column_scale = 0.4 * jnp.exp(jnp.log(6.0) * column)
    values = jnp.clip(jax.random.normal(key, (SEQS, D), jnp.float32), -4.0, 4.0) * column_scale
    return values.astype(jnp.bfloat16)


def shard_levels(key, dims, pieces, least, largest):
    def one(dim, parts):
        steps = jax.random.uniform(jax.random.fold_in(jax.random.fold_in(key, 6), dim), (parts,), jnp.float32, least / len(pieces), largest / len(pieces))
        return jnp.repeat(jnp.exp(steps), dims[dim] // parts).reshape((-1,) + (1,) * (len(dims) - dim - 1))

    factor_of = one(*pieces[0])
    for cut in pieces[1:]:
        factor_of = factor_of * one(*cut)
    return factor_of


def normal_values(stream_key, extent, scale, reach, cuts=(), kind=jnp.bfloat16):
    values = jax.random.normal(stream_key, extent, jnp.float32) * scale
    if len(cuts) > 0:
        values = shard_levels(stream_key, extent, cuts, -0.22, 0.18) * values
    return jnp.clip(values, min=-reach, max=reach).astype(kind)


def setup_inputs(seed: int = 0) -> dict:
    key_of = jax.random.split(jax.random.key(seed), 16)
    tokens = draw_tokens(jax.random.fold_in(key_of[15], 71), 0)
    mix_gain = jnp.clip(1.0 + 0.18 * jax.random.normal(key_of[1], (D,), jnp.float32), 0.099609375, 1.8984375).astype(jnp.bfloat16)
    ffn_gain = jnp.clip(1.0 + 0.18 * jax.random.normal(key_of[2], (D,), jnp.float32), 0.099609375, 1.8984375).astype(jnp.bfloat16)
    w_query = normal_values(key_of[3], (D, HEADS * DK), D ** -0.5, 0.09375, ((0, 16), (1, 2)))
    w_key = normal_values(key_of[4], (D, HEADS * DK), D ** -0.5, 0.09375, ((0, 16), (1, 2)))
    w_value = normal_values(key_of[5], (D, HEADS * DV), D ** -0.5, 0.09375, ((0, 16), (1, 2)))
    w_gate = normal_values(key_of[6], (D, HEADS * DV), D ** -0.5, 0.09375, ((0, 16), (1, 2)))
    w_decay = normal_values(key_of[7], (D, HEADS * DK), (D // 16) ** -0.5, 0.375, ((0, 16), (1, 2)))
    decay_bias = jnp.clip(-7.0 + 11.0 * jax.random.uniform(key_of[8], (HEADS * DK,), jnp.float32) ** shard_levels(key_of[8], (HEADS * DK,), ((0, 2),), -0.2, 0.2), -7.0, 4.0)
    head_gain = jnp.clip(1.0 + 0.18 * jax.random.normal(key_of[9], (DV,), jnp.float32), 0.099609375, 1.8984375).astype(jnp.bfloat16)
    w_output = normal_values(key_of[10], (HEADS * DV, D), (HEADS * DV) ** -0.5, 0.09375, ((0, 2), (1, 16)))
    w_ffgate = normal_values(key_of[11], (D, FF), D ** -0.5, 0.09375, ((0, 16), (1, 2)))
    w_ffup = normal_values(key_of[12], (D, FF), D ** -0.5, 0.09375, ((0, 16), (1, 2)))
    w_down = normal_values(key_of[13], (FF, D), FF ** -0.5, 0.0546875, ((0, 2), (1, 16)))
    state = normal_values(key_of[14], (SEQS, HEADS, DK, DV), 1.0, 6.0, ((0, 16), (1, 2)), jnp.float32)
    return {"tokens": tokens, "mix_gain": mix_gain, "ffn_gain": ffn_gain, "w_query": w_query, "w_key": w_key, "w_value": w_value, "w_gate": w_gate, "w_decay": w_decay, "decay_bias": decay_bias, "head_gain": head_gain, "w_output": w_output, "w_ffgate": w_ffgate, "w_ffup": w_ffup, "w_down": w_down, "state": state}


epsilon = 1e-06

def reference(tokens, mix_gain, ffn_gain, w_query, w_key, w_value, w_gate, w_decay, decay_bias, head_gain, w_output, w_ffgate, w_ffup, w_down, state):
    seq_count = tokens.shape[0]
    model_width = tokens.shape[1]
    head_count = state.shape[1]
    key_dim = state.shape[2]
    val_dim = state.shape[3]
    token_f32 = tokens.astype(jnp.float32)
    mix_rms = lax.rsqrt(lax.optimization_barrier(jnp.sum(token_f32 * token_f32, axis=1)) / model_width + epsilon)[:, None]
    mix_in = (token_f32 * mix_gain.astype(jnp.float32)).astype(jnp.bfloat16)

    def project(weight):
        return jnp.dot(mix_in, weight, preferred_element_type=jnp.float32) * mix_rms
    queries = project(w_query).reshape(seq_count, head_count, key_dim) * key_dim ** (-0.5)
    key_rows = project(w_key).reshape(seq_count, head_count, key_dim)
    value_rows = project(w_value).reshape(seq_count, head_count, val_dim)
    gate_rows = project(w_gate).reshape(seq_count, head_count, val_dim)
    decay_rows = (project(w_decay) + decay_bias).reshape(seq_count, head_count, key_dim)
    log_decay = jax.nn.log_sigmoid(decay_rows) / 16.0
    new_state = jnp.exp(log_decay)[..., None] * state + key_rows[..., :, None] * value_rows[..., None, :]
    attended = jnp.einsum('bhk,bhkv->bhv', queries, new_state, precision=lax.Precision.HIGHEST)
    attended = attended * lax.rsqrt(lax.optimization_barrier(jnp.sum(attended * attended, axis=2, keepdims=True)) / val_dim + epsilon)
    head_out = (attended * head_gain.astype(jnp.float32) * jax.nn.silu(gate_rows)).reshape(seq_count, head_count * val_dim).astype(jnp.bfloat16)
    group_cols = head_count * val_dim // GROUPS
    attn_out = jnp.zeros((seq_count, model_width), jnp.float32)
    for group_idx in range(GROUPS):
        partial_value = jnp.dot(head_out[:, group_idx * group_cols:(group_idx + 1) * group_cols], w_output[group_idx * group_cols:(group_idx + 1) * group_cols], preferred_element_type=jnp.float32)
        attn_out = attn_out + lax.optimization_barrier(partial_value.astype(jnp.bfloat16)).astype(jnp.float32)
    residual_mid = (token_f32 + attn_out).astype(jnp.bfloat16)
    mid_f32 = residual_mid.astype(jnp.float32)
    ffn_rms = lax.rsqrt(lax.optimization_barrier(jnp.sum(mid_f32 * mid_f32, axis=1)) / model_width + epsilon)[:, None]
    ffn_in = (mid_f32 * ffn_gain.astype(jnp.float32)).astype(jnp.bfloat16)
    gate_sum = jnp.dot(ffn_in, w_ffgate, preferred_element_type=jnp.float32)
    up_sum = jnp.dot(ffn_in, w_ffup, preferred_element_type=jnp.float32)
    hidden = (jax.nn.silu(gate_sum * ffn_rms) * (up_sum * ffn_rms)).astype(jnp.bfloat16)
    unit_cols = hidden.shape[1] // GROUPS
    ffn_out = jnp.zeros((seq_count, model_width), jnp.float32)
    for group_idx in range(GROUPS):
        partial_value = jnp.dot(hidden[:, group_idx * unit_cols:(group_idx + 1) * unit_cols], w_down[group_idx * unit_cols:(group_idx + 1) * unit_cols], preferred_element_type=jnp.float32)
        ffn_out = ffn_out + lax.optimization_barrier(partial_value.astype(jnp.bfloat16)).astype(jnp.float32)
    mixed = (mid_f32 + ffn_out).astype(jnp.bfloat16)
    return (mixed, new_state)
```

```python
import functools

import jax
import jax.numpy as jnp
import numpy as np
from jax import lax
from jax.experimental import pallas as pl
from jax.experimental.pallas import tpu as pltpu
from jax.sharding import PartitionSpec as P

epsilon = 1e-06
MESH = pl.DeviceIdType.MESH
LANES = 128
FF_CHUNKS = 4
f32 = jnp.float32
bf16 = jnp.bfloat16


def split_kv(count):
    near = next(n for n in range(1, count + 1) if count % n == 0 and n * n >= count)
    return near, count // near


def ff_bounds(units):
    tiles = units // LANES
    cuts = [(tiles * step + FF_CHUNKS // 2) // FF_CHUNKS * LANES for step in range(FF_CHUNKS + 1)]
    return list(zip(cuts[:-1], cuts[1:]))


def halves(total):
    high = total.astype(bf16)
    low = (total - high.astype(f32)).astype(bf16)
    wide = (total.shape[0], LANES)
    return jnp.concatenate(
        [jnp.broadcast_to(high.astype(f32), wide), jnp.broadcast_to(low.astype(f32), wide)], axis=1
    )


def joined(block):
    return block[:, 0:1] + block[:, LANES : LANES + 1]


def layer_kernel(cfg, *refs):
    near_n, far_n, own, heads, key_dim, val_dim, model_width = cfg["sizes"]
    ins, outs, scratch = refs[:14], refs[14:18], list(refs[18:])
    tokens, params, perm, unperm, w_query, w_key, w_value, w_gate, w_decay = ins[:9]
    w_output, w_ffgate, w_ffup, w_down, state = ins[9:]
    mixed_ref, dec_out, key_out, val_out = outs

    def take(count):
        taken = scratch[:count]
        del scratch[:count]
        return taken

    held = take(10)
    rs_widths, ag_widths = cfg["rs_widths"], cfg["ag_widths"]
    near_out, near_in = take(len(rs_widths)), take(len(rs_widths))
    far_out, far_in = take(len(rs_widths)), take(len(rs_widths))
    ag_far, ag_near = take(len(ag_widths)), take(len(ag_widths))
    stage = take(1)[0]
    swap_out, swap_in = take(2)
    q8, d8, k8, v8, g8, a8 = take(6)
    load_sem, ns_sem, nr_sem, fs_sem, fr_sem = take(5)
    gfs_sem, gfr_sem, gns_sem, gnr_sem, ws_sem, wr_sem = take(6)

    kv = lax.axis_index("kv")
    tp = lax.axis_index("tp")
    near = lax.rem(kv, near_n)
    far = lax.div(kv, near_n)
    block = far_n * own
    rows = near_n * block
    width = tokens.shape[1]

    weights = [w_query, w_decay, w_key, w_value, w_gate, state, w_output, w_ffgate, w_ffup, w_down]
    loads = []
    for index, (source, target) in enumerate(zip(weights, held)):
        load = pltpu.make_async_copy(source, target, load_sem.at[index])
        load.start()
        loads.append(load)
    h_query, h_decay, h_key, h_value, h_gate, h_state, h_output, h_ffgate, h_ffup, h_down = held

    def near_peer(step):
        other = lax.rem(near + step, near_n)
        return other, {"kv": far * near_n + other}

    def far_peer(step):
        other = lax.rem(far + step, far_n)
        return other, {"kv": other * near_n + near}

    barrier = pltpu.get_barrier_semaphore()
    for step in range(1, near_n):
        pl.semaphore_signal(barrier, inc=1, device_id=near_peer(step)[1], device_id_type=MESH)
    for step in range(1, far_n):
        pl.semaphore_signal(barrier, inc=1, device_id=far_peer(step)[1], device_id_type=MESH)
    pl.semaphore_signal(barrier, inc=1, device_id={"tp": 1 - tp}, device_id_type=MESH)

    sent = []

    def send(source, target, send_sem, recv_sem, device):
        copy = pltpu.make_async_remote_copy(
            src_ref=source,
            dst_ref=target,
            send_sem=send_sem,
            recv_sem=recv_sem,
            device_id=device,
            device_id_type=MESH,
        )
        copy.start()
        sent.append(copy)

    def arrived(source, target, send_sem, recv_sem, device):
        pltpu.make_async_remote_copy(
            src_ref=source,
            dst_ref=target,
            send_sem=send_sem,
            recv_sem=recv_sem,
            device_id=device,
            device_id_type=MESH,
        ).wait_recv()

    def put_near(ch, first, value):
        last = first + value.shape[1]
        for other in range(near_n):
            near_out[ch][other, :, first:last] = value[other * block : (other + 1) * block].astype(bf16)

    def start_near(ch):
        for step in range(1, near_n):
            other, device = near_peer(step)
            send(near_out[ch].at[other], near_in[ch].at[near], ns_sem.at[ch, step], nr_sem.at[ch, step], device)

    def sum_near(ch):
        total = near_out[ch][near].astype(f32)
        for step in range(1, near_n):
            origin = lax.rem(near + near_n - step, near_n)
            arrived(
                near_out[ch].at[origin],
                near_in[ch].at[origin],
                ns_sem.at[ch, step],
                nr_sem.at[ch, step],
                {"kv": far * near_n + origin},
            )
            total = total + near_in[ch][origin].astype(f32)
        return total

    def to_far(ch, squares_at=None):
        total = sum_near(ch)
        for other in range(far_n):
            piece = total[other * own : (other + 1) * own]
            if squares_at is None:
                far_out[ch][other] = piece.astype(bf16)
            else:
                far_out[ch][other, :, :squares_at] = piece[:, :squares_at].astype(bf16)
                far_out[ch][other, :, squares_at:] = halves(joined(piece[:, squares_at:])).astype(bf16)
        for step in range(1, far_n):
            other, device = far_peer(step)
            send(far_out[ch].at[other], far_in[ch].at[far], fs_sem.at[ch, step], fr_sem.at[ch, step], device)

    def sum_far(ch):
        total = far_out[ch][far].astype(f32)
        for step in range(1, far_n):
            origin = lax.rem(far + far_n - step, far_n)
            arrived(
                far_out[ch].at[origin],
                far_in[ch].at[origin],
                fs_sem.at[ch, step],
                fr_sem.at[ch, step],
                {"kv": origin * near_n + near},
            )
            total = total + far_in[ch][origin].astype(f32)
        return total

    def start_gather(ch):
        for step in range(1, far_n):
            _, device = far_peer(step)
            send(ag_far[ch].at[far], ag_far[ch].at[far], gfs_sem.at[ch, step], gfr_sem.at[ch, step], device)

    def pass_gather(ch):
        for step in range(1, far_n):
            origin = lax.rem(far + far_n - step, far_n)
            arrived(
                ag_far[ch].at[origin],
                ag_far[ch].at[origin],
                gfs_sem.at[ch, step],
                gfr_sem.at[ch, step],
                {"kv": origin * near_n + near},
            )
        wide = ag_widths[ch]
        for other in range(far_n):
            stage[other * own : (other + 1) * own, :wide] = ag_far[ch][other].astype(f32)
        ag_near[ch][near] = stage[:, :wide].astype(bf16)
        for step in range(1, near_n):
            _, device = near_peer(step)
            send(ag_near[ch].at[near], ag_near[ch].at[near], gns_sem.at[ch, step], gnr_sem.at[ch, step], device)

    def gathered(ch):
        for step in range(1, near_n):
            origin = lax.rem(near + near_n - step, near_n)
            arrived(
                ag_near[ch].at[origin],
                ag_near[ch].at[origin],
                gns_sem.at[ch, step],
                gnr_sem.at[ch, step],
                {"kv": far * near_n + origin},
            )
        return jnp.concatenate([ag_near[ch][other].astype(f32) for other in range(near_n)], axis=0).astype(bf16)

    def over_groups(use, partial):
        swap_out[use] = partial.astype(bf16)
        send(swap_out.at[use], swap_in.at[use], ws_sem.at[use], wr_sem.at[use], {"tp": 1 - tp})
        arrived(swap_out.at[use], swap_in.at[use], ws_sem.at[use], wr_sem.at[use], {"tp": 1 - tp})
        return swap_out[use].astype(f32) + swap_in[use].astype(f32)

    mix_gain = params[:, :width]
    ffn_gain = params[:, width : 2 * width]
    head_gain = params[:, 2 * width : 2 * width + val_dim]
    decay_bias = params[:, 2 * width + val_dim :]

    token_f32 = jnp.dot(perm[...], tokens[...], preferred_element_type=f32)
    mix_in = (token_f32 * mix_gain).astype(bf16)
    attn_channels = ((0, h_query, 0), (1, h_decay, 1), (2, h_key, 2), (3, h_value, 3), (4, h_gate, 4))
    for ch, weight, load in attn_channels:
        loads[load].wait()
        put_near(ch, 0, jnp.dot(mix_in, weight[...], preferred_element_type=f32))
        if ch == 0:
            squares = jnp.sum(token_f32 * token_f32, axis=1, keepdims=True)
            put_near(0, weight.shape[1], halves(squares))
            pl.semaphore_wait(barrier, near_n + far_n - 1)
        start_near(ch)
    key_cols = heads * key_dim
    for ch in range(5):
        to_far(ch, key_cols if ch == 0 else None)

    def by_head(target, wide, value):
        for row in range(own):
            for head in range(heads):
                slot = row * heads + head
                target[slot : slot + 1, :] = value[row : row + 1, head * wide : (head + 1) * wide]

    total = sum_far(0)
    mix_rms = lax.rsqrt(joined(total[:, key_cols:]) / model_width + epsilon)
    by_head(q8, key_dim, total[:, :key_cols] * mix_rms * key_dim ** (-0.5))
    by_head(d8, key_dim, sum_far(1) * mix_rms + decay_bias)
    decay_in = d8[...]
    log_decay = (jnp.minimum(decay_in, 0.0) - jnp.log1p(jnp.exp(-jnp.abs(decay_in)))) / 16.0
    decay = jnp.exp(log_decay)
    dec_out[...] = decay.T
    scaled = (q8[...] * decay).T
    loads[5].wait()
    for row in range(own):
        for head in range(heads):
            slot = row * heads + head
            a8[slot : slot + 1, :] = jnp.sum(h_state[row, head] * scaled[:, slot : slot + 1], axis=0, keepdims=True)
    by_head(k8, key_dim, sum_far(2) * mix_rms)
    key_out[...] = k8[...].T
    by_head(v8, val_dim, sum_far(3) * mix_rms)
    val_out[...] = v8[...]
    by_head(g8, val_dim, sum_far(4) * mix_rms)
    attended = a8[...] + jnp.sum(q8[...] * k8[...], axis=1, keepdims=True) * v8[...]
    attended = attended * lax.rsqrt(jnp.sum(attended * attended, axis=1, keepdims=True) / val_dim + epsilon)
    gates = g8[...]
    a8[...] = attended * head_gain * (gates / (1.0 + jnp.exp(-gates)))
    for row in range(own):
        for head in range(heads):
            slot = row * heads + head
            stage[row : row + 1, head * val_dim : (head + 1) * val_dim] = a8[slot : slot + 1, :]
    ag_far[0][far] = stage[:own, : heads * val_dim].astype(bf16)
    start_gather(0)
    pass_gather(0)
    loads[6].wait()
    head_partial = jnp.dot(gathered(0), h_output[...], preferred_element_type=f32)
    residual_mid = (token_f32 + over_groups(0, head_partial)).astype(bf16)

    mid_f32 = residual_mid.astype(f32)
    ffn_in = (mid_f32 * ffn_gain).astype(bf16)
    bounds = cfg["bounds"]
    loads[7].wait()
    loads[8].wait()
    for index, (low, high) in enumerate(bounds):
        ch = 5 + index
        put_near(ch, 0, jnp.dot(ffn_in, h_ffgate[:, low:high], preferred_element_type=f32))
        put_near(ch, high - low, jnp.dot(ffn_in, h_ffup[:, low:high], preferred_element_type=f32))
        if index == 0:
            put_near(ch, 2 * (high - low), halves(jnp.sum(mid_f32 * mid_f32, axis=1, keepdims=True)))
        start_near(ch)
    loads[9].wait()

    ffn_rms = None
    down = jnp.zeros((rows, width), f32)
    for turn in range(len(bounds) + 3):
        if turn < len(bounds):
            low, high = bounds[turn]
            to_far(5 + turn, 2 * (high - low) if turn == 0 else None)
        index = turn - 1
        if 0 <= index < len(bounds):
            wide = bounds[index][1] - bounds[index][0]
            total = sum_far(5 + index)
            if index == 0:
                ffn_rms = lax.rsqrt(joined(total[:, 2 * wide :]) / model_width + epsilon)
            gate = total[:, :wide] * ffn_rms
            up = total[:, wide : 2 * wide] * ffn_rms
            ag_far[1 + index][far] = (gate / (1.0 + jnp.exp(-gate)) * up).astype(bf16)
            start_gather(1 + index)
        index = turn - 2
        if 0 <= index < len(bounds):
            pass_gather(1 + index)
        index = turn - 3
        if 0 <= index < len(bounds):
            low, high = bounds[index]
            down = down + jnp.dot(gathered(1 + index), h_down[low:high, :], preferred_element_type=f32)
    mixed = (mid_f32 + over_groups(1, down)).astype(bf16)
    mixed_ref[...] = jnp.dot(unperm[...], mixed, preferred_element_type=f32).astype(bf16)
    for copy in sent:
        copy.wait_send()


def state_kernel(decay, keys, values, state, new_state):
    heads = pl.num_programs(1)
    slot = pl.program_id(0) * heads + pl.program_id(1)
    chosen = lax.broadcasted_iota(jnp.int32, decay.shape, 1) == slot
    decay_col = jnp.sum(jnp.where(chosen, decay[...], 0.0), axis=1, keepdims=True)
    key_col = jnp.sum(jnp.where(chosen, keys[...], 0.0), axis=1, keepdims=True)
    new_state[0, 0] = decay_col * state[0, 0] + key_col * values[pl.ds(slot, 1), :]


def local_fused(
    tokens,
    mix_gain,
    ffn_gain,
    w_query,
    w_key,
    w_value,
    w_gate,
    w_decay,
    decay_bias,
    head_gain,
    w_output,
    w_ffgate,
    w_ffup,
    w_down,
    state,
):
    own, heads, key_dim, val_dim = state.shape
    rows, width = tokens.shape
    kv_n = lax.axis_size("kv")
    near_n, far_n = split_kv(kv_n)
    block = far_n * own
    slots = own * heads
    bounds = ff_bounds(w_down.shape[0])
    key_cols, val_cols = heads * key_dim, heads * val_dim
    rs_widths = [key_cols + 2 * LANES, key_cols, key_cols, val_cols, val_cols]
    rs_widths += [2 * (high - low) + (2 * LANES if low == 0 else 0) for low, high in bounds]
    ag_widths = [val_cols] + [high - low for low, high in bounds]
    cfg = {
        "sizes": (near_n, far_n, own, heads, key_dim, val_dim, width * kv_n),
        "rs_widths": rs_widths,
        "ag_widths": ag_widths,
        "bounds": bounds,
    }
    origin = np.arange(rows).reshape(far_n, near_n, own).transpose(1, 0, 2).reshape(-1)
    order = np.zeros((rows, rows), np.float32)
    order[np.arange(rows), origin] = 1.0
    params = jnp.concatenate([mix_gain.astype(f32), ffn_gain.astype(f32), head_gain.astype(f32), decay_bias])[None]
    held = [w_query, w_decay, w_key, w_value, w_gate, state, w_output, w_ffgate, w_ffup, w_down]
    scratch = [pltpu.VMEM(array.shape, array.dtype) for array in held]
    scratch += [pltpu.VMEM((near_n, block, wide), bf16) for wide in rs_widths] * 2
    scratch += [pltpu.VMEM((far_n, own, wide), bf16) for wide in rs_widths] * 2
    scratch += [pltpu.VMEM((far_n, own, wide), bf16) for wide in ag_widths]
    scratch += [pltpu.VMEM((near_n, block, wide), bf16) for wide in ag_widths]
    scratch += [pltpu.VMEM((block, max(ag_widths)), f32)]
    scratch += [pltpu.VMEM((2, rows, width), bf16)] * 2
    scratch += [pltpu.VMEM((slots, wide), f32) for wide in (key_dim, key_dim, key_dim, val_dim, val_dim, val_dim)]
    dma = pltpu.SemaphoreType.DMA
    scratch += [dma((len(held),))]
    scratch += [dma((len(rs_widths), near_n))] * 2 + [dma((len(rs_widths), far_n))] * 2
    scratch += [dma((len(ag_widths), far_n))] * 2 + [dma((len(ag_widths), near_n))] * 2
    scratch += [dma((2,))] * 2
    vmem = pl.BlockSpec(memory_space=pltpu.VMEM)
    hbm = pl.BlockSpec(memory_space=pl.ANY)
    mixed, decay, keys, values = pl.pallas_call(
        functools.partial(layer_kernel, cfg),
        out_shape=(
            jax.ShapeDtypeStruct((rows, width), bf16),
            jax.ShapeDtypeStruct((key_dim, slots), f32),
            jax.ShapeDtypeStruct((key_dim, slots), f32),
            jax.ShapeDtypeStruct((slots, val_dim), f32),
        ),
        in_specs=[vmem] * 4 + [hbm] * 10,
        out_specs=(vmem,) * 4,
        scratch_shapes=scratch,
        compiler_params=pltpu.CompilerParams(
            collective_id=0, has_side_effects=True, vmem_limit_bytes=48 * 1024 * 1024
        ),
    )(
        tokens,
        params,
        jnp.asarray(order, bf16),
        jnp.asarray(order.T, bf16),
        w_query,
        w_key,
        w_value,
        w_gate,
        w_decay,
        w_output,
        w_ffgate,
        w_ffup,
        w_down,
        state,
    )
    whole = pl.BlockSpec((key_dim, slots), lambda row, head: (0, 0))
    tile = pl.BlockSpec((1, 1, key_dim, val_dim), lambda row, head: (row, head, 0, 0))
    new_state = pl.pallas_call(
        state_kernel,
        grid=(own, heads),
        out_shape=jax.ShapeDtypeStruct(state.shape, f32),
        in_specs=[whole, whole, pl.BlockSpec((slots, val_dim), lambda row, head: (0, 0)), tile],
        out_specs=tile,
    )(decay, keys, values, state)
    return (mixed, new_state)


def local_plain(
    tokens,
    mix_gain,
    ffn_gain,
    w_query,
    w_key,
    w_value,
    w_gate,
    w_decay,
    decay_bias,
    head_gain,
    w_output,
    w_ffgate,
    w_ffup,
    w_down,
    state,
):
    own_rows = state.shape[0]
    local_heads = state.shape[1]
    key_dim = state.shape[2]
    val_dim = state.shape[3]
    model_width = tokens.shape[1] * lax.axis_size("kv")
    row_offset = lax.axis_index("kv") * own_rows
    token_f32 = tokens.astype(jnp.float32)
    row_squares = jnp.sum(token_f32 * token_f32, axis=1)
    mix_in = (token_f32 * mix_gain.astype(jnp.float32)).astype(jnp.bfloat16)
    query_part = jnp.dot(mix_in, w_query, preferred_element_type=jnp.float32)
    key_part = jnp.dot(mix_in, w_key, preferred_element_type=jnp.float32)
    value_part = jnp.dot(mix_in, w_value, preferred_element_type=jnp.float32)
    gate_part = jnp.dot(mix_in, w_gate, preferred_element_type=jnp.float32)
    decay_part = jnp.dot(mix_in, w_decay, preferred_element_type=jnp.float32)
    square_total = lax.psum(row_squares, "kv")
    own_squares = lax.dynamic_slice_in_dim(square_total, row_offset, own_rows)
    query_sum, key_sum, value_sum, gate_sum, decay_sum = (
        lax.psum_scatter(query_part, "kv", scatter_dimension=0, tiled=True),
        lax.psum_scatter(key_part, "kv", scatter_dimension=0, tiled=True),
        lax.psum_scatter(value_part, "kv", scatter_dimension=0, tiled=True),
        lax.psum_scatter(gate_part, "kv", scatter_dimension=0, tiled=True),
        lax.psum_scatter(decay_part, "kv", scatter_dimension=0, tiled=True),
    )
    mix_rms = lax.rsqrt(own_squares / model_width + epsilon)[:, None]
    queries = (query_sum * mix_rms).reshape(own_rows, local_heads, key_dim) * key_dim ** (-0.5)
    key_rows = (key_sum * mix_rms).reshape(own_rows, local_heads, key_dim)
    value_rows = (value_sum * mix_rms).reshape(own_rows, local_heads, val_dim)
    gate_rows = (gate_sum * mix_rms).reshape(own_rows, local_heads, val_dim)
    decay_rows = (decay_sum * mix_rms + decay_bias).reshape(own_rows, local_heads, key_dim)
    log_decay = jax.nn.log_sigmoid(decay_rows) / 16.0
    new_state = (
        jnp.exp(log_decay)[..., None] * state + key_rows[..., :, None] * value_rows[..., None, :]
    )
    attended = jnp.einsum("bhk,bhkv->bhv", queries, new_state, precision=lax.Precision.HIGHEST)
    attended = attended * lax.rsqrt(
        jnp.sum(attended * attended, axis=2, keepdims=True) / val_dim + epsilon
    )
    head_out = (
        (attended * head_gain.astype(jnp.float32) * jax.nn.silu(gate_rows))
        .reshape(own_rows, local_heads * val_dim)
        .astype(jnp.bfloat16)
    )
    head_partial = jnp.dot(
        lax.all_gather(head_out, "kv", axis=0, tiled=True),
        w_output,
        preferred_element_type=jnp.float32,
    )
    attn_out = lax.psum(head_partial.astype(jnp.bfloat16), "tp").astype(jnp.float32)
    residual_mid = (token_f32 + attn_out).astype(jnp.bfloat16)
    mid_f32 = residual_mid.astype(jnp.float32)
    mid_squares = jnp.sum(mid_f32 * mid_f32, axis=1)
    ffn_in = (mid_f32 * ffn_gain.astype(jnp.float32)).astype(jnp.bfloat16)
    ffgate_part = jnp.dot(ffn_in, w_ffgate, preferred_element_type=jnp.float32)
    ffup_part = jnp.dot(ffn_in, w_ffup, preferred_element_type=jnp.float32)
    ffgate_sum, ffup_sum, square_sum = lax.psum((ffgate_part, ffup_part, mid_squares), "kv")
    ffn_rms = lax.rsqrt(square_sum / model_width + epsilon)[:, None]
    hidden = (jax.nn.silu(ffgate_sum * ffn_rms) * (ffup_sum * ffn_rms)).astype(jnp.bfloat16)
    down_part = jnp.dot(hidden, w_down, preferred_element_type=jnp.float32)
    ffn_out = lax.psum(down_part.astype(jnp.bfloat16), "tp").astype(jnp.float32)
    mixed = (mid_f32 + ffn_out).astype(jnp.bfloat16)
    return (mixed, new_state)


def fits(tokens, w_query, w_down, state):
    own, heads, key_dim, val_dim = state.shape
    near_n, far_n = split_kv(lax.axis_size("kv"))
    return (
        lax.axis_size("tp") == 2
        and near_n > 1
        and far_n > 1
        and (far_n * own) % 8 == 0
        and (own * heads) % 8 == 0
        and all(extent % LANES == 0 for extent in (tokens.shape[1], key_dim, val_dim, w_down.shape[0]))
        and w_down.shape[0] // LANES >= FF_CHUNKS
    )


def local(*arrays):
    tokens, w_query, w_down, state = arrays[0], arrays[3], arrays[13], arrays[14]
    if fits(tokens, w_query, w_down, state):
        return local_fused(*arrays)
    return local_plain(*arrays)


def solution(mesh):
    in_specs = (
        P(None, "kv"),
        P("kv"),
        P("kv"),
        P("kv", "tp"),
        P("kv", "tp"),
        P("kv", "tp"),
        P("kv", "tp"),
        P("kv", "tp"),
        P("tp"),
        P(),
        P("tp", "kv"),
        P("kv", "tp"),
        P("kv", "tp"),
        P("tp", "kv"),
        P("kv", "tp", None, None),
    )
    out_specs = (P(None, "kv"), P("kv", "tp", None, None))
    return jax.shard_map(local, mesh=mesh, in_specs=in_specs, out_specs=out_specs, check_vma=False)
```

```python
import functools

import jax
import jax.numpy as jnp
import numpy as np
from jax import lax
from jax.experimental import pallas as pl
from jax.experimental.pallas import tpu as pltpu
from jax.sharding import PartitionSpec as P

epsilon = 1e-06
MESH = pl.DeviceIdType.MESH
LANES = 128
FF_CHUNKS = 3
LAGS = (1, 2, 3)
ATTN_CHANNELS = (("query", "decay", "key"), ("value",), ("gate",))
VMEM_BYTES = 67043328
f32 = jnp.float32
bf16 = jnp.bfloat16


def split_kv(count):
    near = next(n for n in range(1, count + 1) if count % n == 0 and n * n >= count)
    return near, count // near


def ff_bounds(units):
    tiles = units // LANES
    cuts = [(tiles * step + FF_CHUNKS // 2) // FF_CHUNKS * LANES for step in range(FF_CHUNKS + 1)]
    return list(zip(cuts[:-1], cuts[1:]))


def halves(total):
    high = total.astype(bf16)
    low = (total - high.astype(f32)).astype(bf16)
    wide = (total.shape[0], LANES)
    return jnp.concatenate(
        [jnp.broadcast_to(high.astype(f32), wide), jnp.broadcast_to(low.astype(f32), wide)], axis=1
    )


def joined(block):
    return block[:, 0:1] + block[:, LANES : LANES + 1]


def layer_kernel(cfg, *refs):
    near_n, far_n, own, heads, key_dim, val_dim, model_width = cfg["sizes"]
    ins, outs, scratch = refs[:15], refs[15:17], list(refs[17:])
    mixed_ref, new_state = outs

    def take(count):
        taken = scratch[:count]
        del scratch[:count]
        return taken

    held = take(15)
    rs_widths, ag_widths = cfg["rs_widths"], cfg["ag_widths"]
    near_out, near_in = take(len(rs_widths)), take(len(rs_widths))
    far_out, far_in = take(len(rs_widths)), take(len(rs_widths))
    ag_far, ag_near = take(len(ag_widths)), take(len(ag_widths))
    stage = take(1)[0]
    swap_out, swap_in = take(2)
    q8, d8, k8, v8, g8, a8 = take(6)
    made = take(1)[0]
    load_sem, ns_sem, nr_sem, fs_sem, fr_sem = take(5)
    gfs_sem, gfr_sem, gns_sem, gnr_sem, ws_sem, wr_sem = take(6)
    out_sem = take(1)[0]

    kv = lax.axis_index("kv")
    tp = lax.axis_index("tp")
    near = lax.rem(kv, near_n)
    far = lax.div(kv, near_n)
    block = far_n * own
    rows = near_n * block
    width = ins[0].shape[1]

    loads = []
    for index, (source, target) in enumerate(zip(ins, held)):
        load = pltpu.make_async_copy(source, target, load_sem.at[index])
        load.start()
        loads.append(load)
    tokens, mix_ref, h_query, h_decay, h_key, bias_ref, h_value, h_gate = held[:8]
    h_state, head_ref, ffn_ref, h_output, h_ffgate, h_ffup, h_down = held[8:]

    pair = 2 if near_n % 2 == 0 else 1
    shifts = [(a, b) for a in range(pair) for b in range(near_n // pair)]
    shifts.sort(key=lambda shift: (shift != (0, 0), -(shift[0] > 0) - (shift[1] > 0)))

    def near_shift(step, back=1):
        a, b = shifts[step]
        deep = near_n // pair
        low = lax.rem(lax.rem(near, pair) + pair + back * a, pair)
        high = lax.rem(lax.div(near, pair) + deep + back * b, deep)
        return high * pair + low

    def near_peer(step):
        other = near_shift(step)
        return other, {"kv": far * near_n + other}

    def far_peer(step):
        other = lax.rem(far + step, far_n)
        return other, {"kv": other * near_n + near}

    barrier = pltpu.get_barrier_semaphore()
    for step in range(1, near_n):
        pl.semaphore_signal(barrier, inc=1, device_id=near_peer(step)[1], device_id_type=MESH)
    for step in range(1, far_n):
        pl.semaphore_signal(barrier, inc=1, device_id=far_peer(step)[1], device_id_type=MESH)
    pl.semaphore_signal(barrier, inc=1, device_id={"tp": 1 - tp}, device_id_type=MESH)

    sent = []

    def send(source, target, send_sem, recv_sem, device):
        copy = pltpu.make_async_remote_copy(
            src_ref=source,
            dst_ref=target,
            send_sem=send_sem,
            recv_sem=recv_sem,
            device_id=device,
            device_id_type=MESH,
        )
        copy.start()
        sent.append(copy)

    def arrived(source, target, send_sem, recv_sem, device):
        pltpu.make_async_remote_copy(
            src_ref=source,
            dst_ref=target,
            send_sem=send_sem,
            recv_sem=recv_sem,
            device_id=device,
            device_id_type=MESH,
        ).wait_recv()

    def put_near(ch, first, value):
        last = first + value.shape[1]
        for other in range(near_n):
            near_out[ch][other, :, first:last] = value[other * block : (other + 1) * block].astype(bf16)

    def start_near(ch):
        for step in range(1, near_n):
            other, device = near_peer(step)
            send(near_out[ch].at[other], near_in[ch].at[near], ns_sem.at[ch, step], nr_sem.at[ch, step], device)

    def sum_near(ch):
        total = near_out[ch][near].astype(f32)
        for step in range(1, near_n):
            origin = near_shift(step, -1)
            arrived(
                near_out[ch].at[origin],
                near_in[ch].at[origin],
                ns_sem.at[ch, step],
                nr_sem.at[ch, step],
                {"kv": far * near_n + origin},
            )
            total = total + near_in[ch][origin].astype(f32)
        return total

    def to_far(ch, squares_at=None):
        total = sum_near(ch)
        for other in range(far_n):
            piece = total[other * own : (other + 1) * own]
            if squares_at is None:
                far_out[ch][other] = piece.astype(bf16)
            else:
                far_out[ch][other, :, :squares_at] = piece[:, :squares_at].astype(bf16)
                far_out[ch][other, :, squares_at:] = halves(joined(piece[:, squares_at:])).astype(bf16)
        for step in range(1, far_n):
            other, device = far_peer(step)
            send(far_out[ch].at[other], far_in[ch].at[far], fs_sem.at[ch, step], fr_sem.at[ch, step], device)

    def sum_far(ch):
        total = far_out[ch][far].astype(f32)
        for step in range(1, far_n):
            origin = lax.rem(far + far_n - step, far_n)
            arrived(
                far_out[ch].at[origin],
                far_in[ch].at[origin],
                fs_sem.at[ch, step],
                fr_sem.at[ch, step],
                {"kv": origin * near_n + near},
            )
            total = total + far_in[ch][origin].astype(f32)
        return total

    def start_gather(ch):
        for step in range(1, far_n):
            _, device = far_peer(step)
            send(ag_far[ch].at[far], ag_far[ch].at[far], gfs_sem.at[ch, step], gfr_sem.at[ch, step], device)

    def pass_gather(ch):
        for step in range(1, far_n):
            origin = lax.rem(far + far_n - step, far_n)
            arrived(
                ag_far[ch].at[origin],
                ag_far[ch].at[origin],
                gfs_sem.at[ch, step],
                gfr_sem.at[ch, step],
                {"kv": origin * near_n + near},
            )
        wide = ag_widths[ch]
        for other in range(far_n):
            stage[other * own : (other + 1) * own, :wide] = ag_far[ch][other].astype(f32)
        ag_near[ch][near] = stage[:, :wide].astype(bf16)
        for step in range(1, near_n):
            _, device = near_peer(step)
            send(ag_near[ch].at[near], ag_near[ch].at[near], gns_sem.at[ch, step], gnr_sem.at[ch, step], device)

    def gathered(ch):
        for step in range(1, near_n):
            origin = near_shift(step, -1)
            arrived(
                ag_near[ch].at[origin],
                ag_near[ch].at[origin],
                gns_sem.at[ch, step],
                gnr_sem.at[ch, step],
                {"kv": far * near_n + origin},
            )
        return jnp.concatenate([ag_near[ch][other].astype(f32) for other in range(near_n)], axis=0).astype(bf16)

    def over_groups(use, partial):
        swap_out[use] = partial.astype(bf16)
        send(swap_out.at[use], swap_in.at[use], ws_sem.at[use], wr_sem.at[use], {"tp": 1 - tp})
        arrived(swap_out.at[use], swap_in.at[use], ws_sem.at[use], wr_sem.at[use], {"tp": 1 - tp})
        return swap_out[use].astype(f32) + swap_in[use].astype(f32)

    def gain(ref):
        return ref[...].astype(f32).reshape(1, -1)

    row_at = lax.broadcasted_iota(jnp.int32, (rows, rows), 0)
    col_at = lax.broadcasted_iota(jnp.int32, (rows, rows), 1)
    perm = jnp.zeros((rows, rows), f32)
    unperm = jnp.zeros((rows, rows), f32)
    for slot, origin in enumerate(cfg["order"]):
        perm = jnp.where((row_at == slot) & (col_at == origin), 1.0, perm)
        unperm = jnp.where((col_at == slot) & (row_at == origin), 1.0, unperm)
    loads[0].wait()
    loads[1].wait()
    token_f32 = jnp.dot(perm.astype(bf16), tokens[...], preferred_element_type=f32)
    mix_in = (token_f32 * gain(mix_ref)).astype(bf16)
    first = {}
    squares = halves(jnp.sum(token_f32 * token_f32, axis=1, keepdims=True))
    weight_at = {"query": 2, "decay": 3, "key": 4, "value": 6, "gate": 7}
    for ch, names in enumerate(ATTN_CHANNELS):
        at = 0
        for name in names:
            weight = held[weight_at[name]]
            loads[weight_at[name]].wait()
            put_near(ch, at, jnp.dot(mix_in, weight[...], preferred_element_type=f32))
            first[name] = (ch, at, at + weight.shape[1])
            at += weight.shape[1]
        if ch == 0:
            put_near(0, at, squares)
            squares_at = at
            pl.semaphore_wait(barrier, near_n + far_n - 1)
        start_near(ch)
    for ch in range(len(ATTN_CHANNELS)):
        to_far(ch, squares_at if ch == 0 else None)
    totals = {}

    def projected(name):
        ch, low, high = first[name]
        if ch not in totals:
            totals[ch] = sum_far(ch)
        return totals[ch][:, low:high]

    def by_head(target, wide, value):
        for row in range(own):
            for head in range(heads):
                slot = row * heads + head
                target[slot : slot + 1, :] = value[row : row + 1, head * wide : (head + 1) * wide]

    loads[5].wait()
    totals[0] = sum_far(0)
    mix_rms = lax.rsqrt(joined(totals[0][:, squares_at:]) / model_width + epsilon)
    by_head(q8, key_dim, projected("query") * mix_rms * key_dim ** (-0.5))
    by_head(d8, key_dim, projected("decay") * mix_rms + gain(bias_ref))
    decay_in = d8[...]
    log_decay = (jnp.minimum(decay_in, 0.0) - jnp.log1p(jnp.exp(-jnp.abs(decay_in)))) / 16.0
    decay = jnp.exp(log_decay)
    decay_cols = decay.T
    scaled = (q8[...] * decay).T
    loads[8].wait()
    for row in range(own):
        for head in range(heads):
            slot = row * heads + head
            a8[slot : slot + 1, :] = jnp.sum(h_state[row, head] * scaled[:, slot : slot + 1], axis=0, keepdims=True)
    by_head(k8, key_dim, projected("key") * mix_rms)
    key_cols_t = k8[...].T
    by_head(v8, val_dim, projected("value") * mix_rms)
    by_head(g8, val_dim, projected("gate") * mix_rms)
    attended = a8[...] + jnp.sum(q8[...] * k8[...], axis=1, keepdims=True) * v8[...]
    attended = attended * lax.rsqrt(jnp.sum(attended * attended, axis=1, keepdims=True) / val_dim + epsilon)
    gates = g8[...]
    loads[9].wait()
    a8[...] = attended * gain(head_ref) * (gates / (1.0 + jnp.exp(-gates)))
    for row in range(own):
        for head in range(heads):
            slot = row * heads + head
            stage[row : row + 1, head * val_dim : (head + 1) * val_dim] = a8[slot : slot + 1, :]
    ag_far[0][far] = stage[:own, : heads * val_dim].astype(bf16)
    start_gather(0)
    for row in range(own):
        for head in range(heads):
            slot = row * heads + head
            made[row, head] = (
                decay_cols[:, slot : slot + 1] * h_state[row, head]
                + key_cols_t[:, slot : slot + 1] * v8[slot : slot + 1, :]
            )
    store = pltpu.make_async_copy(made, new_state, out_sem)
    store.start()
    pass_gather(0)
    loads[11].wait()
    head_partial = jnp.dot(gathered(0), h_output[...], preferred_element_type=f32)
    residual_mid = (token_f32 + over_groups(0, head_partial)).astype(bf16)

    mid_f32 = residual_mid.astype(f32)
    loads[10].wait()
    ffn_in = (mid_f32 * gain(ffn_ref)).astype(bf16)
    bounds = cfg["bounds"]
    ff_first = len(ATTN_CHANNELS)
    loads[12].wait()
    loads[13].wait()
    for index, (low, high) in enumerate(bounds):
        ch = ff_first + index
        put_near(ch, 0, jnp.dot(ffn_in, h_ffgate[:, low:high], preferred_element_type=f32))
        put_near(ch, high - low, jnp.dot(ffn_in, h_ffup[:, low:high], preferred_element_type=f32))
        if index == 0:
            put_near(ch, 2 * (high - low), halves(jnp.sum(mid_f32 * mid_f32, axis=1, keepdims=True)))
        start_near(ch)
    loads[14].wait()

    ffn_rms = None
    down = jnp.zeros((rows, width), f32)
    for turn in range(len(bounds) + LAGS[2]):
        if turn < len(bounds):
            low, high = bounds[turn]
            to_far(ff_first + turn, 2 * (high - low) if turn == 0 else None)
        index = turn - LAGS[0]
        if 0 <= index < len(bounds):
            wide = bounds[index][1] - bounds[index][0]
            total = sum_far(ff_first + index)
            if index == 0:
                ffn_rms = lax.rsqrt(joined(total[:, 2 * wide :]) / model_width + epsilon)
            gate = total[:, :wide] * ffn_rms
            up = total[:, wide : 2 * wide] * ffn_rms
            ag_far[1 + index][far] = (gate / (1.0 + jnp.exp(-gate)) * up).astype(bf16)
            start_gather(1 + index)
        index = turn - LAGS[1]
        if 0 <= index < len(bounds):
            pass_gather(1 + index)
        index = turn - LAGS[2]
        if 0 <= index < len(bounds):
            low, high = bounds[index]
            down = down + jnp.dot(gathered(1 + index), h_down[low:high, :], preferred_element_type=f32)
    mixed = (mid_f32 + over_groups(1, down)).astype(bf16)
    mixed_ref[...] = jnp.dot(unperm.astype(bf16), mixed, preferred_element_type=f32).astype(bf16)
    for copy in sent:
        copy.wait_send()
    store.wait()


def hand_over(mixed_in, state_in, mixed_out, state_out, mixed_held, state_held, in_sem, out_sem):
    own, heads = state_in.shape[:2]
    places = [(row, head) for row in range(own) for head in range(heads)]
    moves = [(mixed_in, mixed_held, mixed_out)]
    moves += [(state_in.at[place], state_held.at[place], state_out.at[place]) for place in places]
    loads = [pltpu.make_async_copy(move[0], move[1], in_sem.at[slot]) for slot, move in enumerate(moves)]
    stores = [pltpu.make_async_copy(move[1], move[2], out_sem.at[slot]) for slot, move in enumerate(moves)]
    for load in loads:
        load.start()
    for load, store in zip(loads, stores):
        load.wait()
        store.start()
    for store in stores:
        store.wait()


def local_fused(
    tokens,
    mix_gain,
    ffn_gain,
    w_query,
    w_key,
    w_value,
    w_gate,
    w_decay,
    decay_bias,
    head_gain,
    w_output,
    w_ffgate,
    w_ffup,
    w_down,
    state,
):
    own, heads, key_dim, val_dim = state.shape
    rows, width = tokens.shape
    kv_n = lax.axis_size("kv")
    near_n, far_n = split_kv(kv_n)
    block = far_n * own
    slots = own * heads
    bounds = ff_bounds(w_down.shape[0])
    key_cols, val_cols = heads * key_dim, heads * val_dim
    extents = {"query": key_cols, "decay": key_cols, "key": key_cols, "value": val_cols, "gate": val_cols}
    rs_widths = [sum(extents[name] for name in names) for names in ATTN_CHANNELS]
    rs_widths[0] += 2 * LANES
    rs_widths += [2 * (high - low) + (2 * LANES if low == 0 else 0) for low, high in bounds]
    ag_widths = [val_cols] + [high - low for low, high in bounds]
    cfg = {
        "sizes": (near_n, far_n, own, heads, key_dim, val_dim, width * kv_n),
        "rs_widths": rs_widths,
        "ag_widths": ag_widths,
        "bounds": bounds,
        "order": np.arange(rows).reshape(far_n, near_n, own).transpose(1, 0, 2).reshape(-1).tolist(),
    }
    held = [tokens, mix_gain, w_query, w_decay, w_key, decay_bias, w_value, w_gate, state]
    held += [head_gain, ffn_gain, w_output, w_ffgate, w_ffup, w_down]
    scratch = [pltpu.VMEM(array.shape, array.dtype) for array in held]
    scratch += [pltpu.VMEM((near_n, block, wide), bf16) for wide in rs_widths] * 2
    scratch += [pltpu.VMEM((far_n, own, wide), bf16) for wide in rs_widths] * 2
    scratch += [pltpu.VMEM((far_n, own, wide), bf16) for wide in ag_widths]
    scratch += [pltpu.VMEM((near_n, block, wide), bf16) for wide in ag_widths]
    scratch += [pltpu.VMEM((block, max(ag_widths)), f32)]
    scratch += [pltpu.VMEM((2, rows, width), bf16)] * 2
    scratch += [pltpu.VMEM((slots, wide), f32) for wide in (key_dim, key_dim, key_dim, val_dim, val_dim, val_dim)]
    scratch += [pltpu.VMEM(state.shape, f32)]
    dma = pltpu.SemaphoreType.DMA
    scratch += [dma((15,))]
    scratch += [dma((len(rs_widths), near_n))] * 2 + [dma((len(rs_widths), far_n))] * 2
    scratch += [dma((len(ag_widths), far_n))] * 2 + [dma((len(ag_widths), near_n))] * 2
    scratch += [dma((2,))] * 2
    scratch += [dma]
    vmem = pl.BlockSpec(memory_space=pltpu.VMEM)
    hbm = pl.BlockSpec(memory_space=pltpu.HBM)
    results = pl.pallas_call(
        functools.partial(layer_kernel, cfg),
        out_shape=(jax.ShapeDtypeStruct((rows, width), bf16), jax.ShapeDtypeStruct(state.shape, f32)),
        in_specs=[hbm] * len(held),
        out_specs=(vmem, hbm),
        scratch_shapes=scratch,
        compiler_params=pltpu.CompilerParams(
            collective_id=0, has_side_effects=True, vmem_limit_bytes=VMEM_BYTES
        ),
    )(*held)
    dma = pltpu.SemaphoreType.DMA
    return pl.pallas_call(
        hand_over,
        out_shape=(jax.ShapeDtypeStruct((rows, width), bf16), jax.ShapeDtypeStruct(state.shape, f32)),
        in_specs=[hbm] * 2,
        out_specs=(hbm,) * 2,
        scratch_shapes=[
            pltpu.VMEM((rows, width), bf16),
            pltpu.VMEM(state.shape, f32),
            dma((1 + slots,)),
            dma((1 + slots,)),
        ],
        compiler_params=pltpu.CompilerParams(vmem_limit_bytes=VMEM_BYTES),
    )(*results)


def local_plain(
    tokens,
    mix_gain,
    ffn_gain,
    w_query,
    w_key,
    w_value,
    w_gate,
    w_decay,
    decay_bias,
    head_gain,
    w_output,
    w_ffgate,
    w_ffup,
    w_down,
    state,
):
    own_rows = state.shape[0]
    local_heads = state.shape[1]
    key_dim = state.shape[2]
    val_dim = state.shape[3]
    model_width = tokens.shape[1] * lax.axis_size("kv")
    row_offset = lax.axis_index("kv") * own_rows
    token_f32 = tokens.astype(jnp.float32)
    row_squares = jnp.sum(token_f32 * token_f32, axis=1)
    mix_in = (token_f32 * mix_gain.astype(jnp.float32)).astype(jnp.bfloat16)
    query_part = jnp.dot(mix_in, w_query, preferred_element_type=jnp.float32)
    key_part = jnp.dot(mix_in, w_key, preferred_element_type=jnp.float32)
    value_part = jnp.dot(mix_in, w_value, preferred_element_type=jnp.float32)
    gate_part = jnp.dot(mix_in, w_gate, preferred_element_type=jnp.float32)
    decay_part = jnp.dot(mix_in, w_decay, preferred_element_type=jnp.float32)
    square_total = lax.psum(row_squares, "kv")
    own_squares = lax.dynamic_slice_in_dim(square_total, row_offset, own_rows)
    query_sum, key_sum, value_sum, gate_sum, decay_sum = (
        lax.psum_scatter(query_part, "kv", scatter_dimension=0, tiled=True),
        lax.psum_scatter(key_part, "kv", scatter_dimension=0, tiled=True),
        lax.psum_scatter(value_part, "kv", scatter_dimension=0, tiled=True),
        lax.psum_scatter(gate_part, "kv", scatter_dimension=0, tiled=True),
        lax.psum_scatter(decay_part, "kv", scatter_dimension=0, tiled=True),
    )
    mix_rms = lax.rsqrt(own_squares / model_width + epsilon)[:, None]
    queries = (query_sum * mix_rms).reshape(own_rows, local_heads, key_dim) * key_dim ** (-0.5)
    key_rows = (key_sum * mix_rms).reshape(own_rows, local_heads, key_dim)
    value_rows = (value_sum * mix_rms).reshape(own_rows, local_heads, val_dim)
    gate_rows = (gate_sum * mix_rms).reshape(own_rows, local_heads, val_dim)
    decay_rows = (decay_sum * mix_rms + decay_bias).reshape(own_rows, local_heads, key_dim)
    log_decay = jax.nn.log_sigmoid(decay_rows) / 16.0
    new_state = (
        jnp.exp(log_decay)[..., None] * state + key_rows[..., :, None] * value_rows[..., None, :]
    )
    attended = jnp.einsum("bhk,bhkv->bhv", queries, new_state, precision=lax.Precision.HIGHEST)
    attended = attended * lax.rsqrt(
        jnp.sum(attended * attended, axis=2, keepdims=True) / val_dim + epsilon
    )
    head_out = (
        (attended * head_gain.astype(jnp.float32) * jax.nn.silu(gate_rows))
        .reshape(own_rows, local_heads * val_dim)
        .astype(jnp.bfloat16)
    )
    head_partial = jnp.dot(
        lax.all_gather(head_out, "kv", axis=0, tiled=True),
        w_output,
        preferred_element_type=jnp.float32,
    )
    attn_out = lax.psum(head_partial.astype(jnp.bfloat16), "tp").astype(jnp.float32)
    residual_mid = (token_f32 + attn_out).astype(jnp.bfloat16)
    mid_f32 = residual_mid.astype(jnp.float32)
    mid_squares = jnp.sum(mid_f32 * mid_f32, axis=1)
    ffn_in = (mid_f32 * ffn_gain.astype(jnp.float32)).astype(jnp.bfloat16)
    ffgate_part = jnp.dot(ffn_in, w_ffgate, preferred_element_type=jnp.float32)
    ffup_part = jnp.dot(ffn_in, w_ffup, preferred_element_type=jnp.float32)
    ffgate_sum, ffup_sum, square_sum = lax.psum((ffgate_part, ffup_part, mid_squares), "kv")
    ffn_rms = lax.rsqrt(square_sum / model_width + epsilon)[:, None]
    hidden = (jax.nn.silu(ffgate_sum * ffn_rms) * (ffup_sum * ffn_rms)).astype(jnp.bfloat16)
    down_part = jnp.dot(hidden, w_down, preferred_element_type=jnp.float32)
    ffn_out = lax.psum(down_part.astype(jnp.bfloat16), "tp").astype(jnp.float32)
    mixed = (mid_f32 + ffn_out).astype(jnp.bfloat16)
    return (mixed, new_state)


def fits(tokens, w_query, w_down, state):
    own, heads, key_dim, val_dim = state.shape
    near_n, far_n = split_kv(lax.axis_size("kv"))
    return (
        lax.axis_size("tp") == 2
        and near_n > 1
        and far_n > 1
        and (far_n * own) % 8 == 0
        and (own * heads) % 8 == 0
        and all(extent % LANES == 0 for extent in (tokens.shape[1], key_dim, val_dim, w_down.shape[0]))
        and w_down.shape[0] // LANES >= FF_CHUNKS
    )


def local(*arrays):
    tokens, w_query, w_down, state = arrays[0], arrays[3], arrays[13], arrays[14]
    if fits(tokens, w_query, w_down, state):
        return local_fused(*arrays)
    return local_plain(*arrays)


def solution(mesh):
    in_specs = (
        P(None, "kv"),
        P("kv"),
        P("kv"),
        P("kv", "tp"),
        P("kv", "tp"),
        P("kv", "tp"),
        P("kv", "tp"),
        P("kv", "tp"),
        P("tp"),
        P(),
        P("tp", "kv"),
        P("kv", "tp"),
        P("kv", "tp"),
        P("tp", "kv"),
        P("kv", "tp", None, None),
    )
    out_specs = (P(None, "kv"), P("kv", "tp", None, None))
    return jax.shard_map(local, mesh=mesh, in_specs=in_specs, out_specs=out_specs, check_vma=False)
```
